512 devices in a mesh: gr: 2 (over z_hi), sp: 32 (over z_lo, y), tp: 8 (over x, core).
Axes of the slice: x: 4, y: 4, z: 16 (z_hi: 2, z_lo: 8; z = z_hi * 8 + z_lo), core: 2. Of those that a mesh axis runs over, the one named last changes fastest.
Arguments:
- tokens: bfloat16 [4, 32768, 2048], P('gr', ('sp', 'tp')), parts along dimension 0, may hold values from -6 to 6
- key_weight: bfloat16 [2048, 1024], P('sp'), may hold values from -0.125 to 0.125
- value_weight: bfloat16 [2048, 1024], P('sp'), may hold values from -0.125 to 0.125
- queries: bfloat16 [4, 1024], P('gr'), parts along dimension 0, may hold values from -6 to 6
- head_offset: float32 [16], replicated, may hold values from -14 to -3.5
- key_bias: bfloat16 [4, 32768, 16], P('gr', ('sp', 'tp')), parts along dimension 0, may hold values from -0.5 to 12.9
Outputs:
- key_cache: bfloat16 [4, 32768, 1024], P('gr', 'sp', 'tp'), parts along dimension 0
- value_cache: bfloat16 [4, 32768, 1024], P('gr', 'sp', 'tp'), parts along dimension 0
- bias_cache: bfloat16 [4, 32768, 16], P('gr', 'sp', 'tp'), parts along dimension 0
- reading: float32 [4, 1024], P('gr', 'tp'), parts along dimension 0
The draws below stay inside these ranges and needn't reach their ends.
There are 2 independent parts, one for each index of `gr`. The reference program is written for one: setup_inputs(seed, part) draws one part's arguments, and reference() takes and returns one part's arrays. A program takes and returns all parts, laid end to end along the dimension named above; an argument that names none is the same for every part. Nothing has to cross between parts.
All inputs are finite; a program needn't handle non-finite values.
Results may differ from the reference program's by a relative error of at most 0.0052.
Values may be sent and summed in bfloat16 or wider, within the bound.
A program may use at most 64 MiB of HBM per device.

```python
import jax
import jax.numpy as jnp
from jax import lax

D = 2048
HEADS = 16
HEAD_DIM = 64
GROUP_SEQUENCES = 2
POS_DEV = 128
PROMPT_LENGTH = 32768


def draw_head_offset(key, part):
    key_a, key_b, key_c, order_key = jax.random.split(jax.random.fold_in(key, 11), 4)
    scale_base = jnp.log(jnp.float32(PROMPT_LENGTH) * 14.6)
    slow_rate = jnp.log(jax.random.uniform(key_a, (HEADS,), jnp.float32, 1.0, 2.3)) - scale_base
    middle_rate = jnp.log(jax.random.uniform(key_c, (HEADS,), jnp.float32, 5.0, 9.0)) - scale_base
    fast_rate = jax.random.uniform(key_b, (HEADS,), jnp.float32, -5.0, -3.5)
    ranks = jax.random.permutation(order_key, HEADS)
    chosen = jnp.where(ranks < HEADS // 2, slow_rate, jnp.where(ranks < 3 * HEADS // 4, middle_rate, fast_rate))
    return chosen.astype(jnp.float32)


def draw_key_bias(key, part):
    key_a, key_b, third_random_key, fourth_random_key = jax.random.split(jax.random.fold_in(key, 23), 4)
    block_count = PROMPT_LENGTH // POS_DEV
    block_tier = jax.random.uniform(key_a, (GROUP_SEQUENCES, block_count, 1, HEADS), jnp.float32, 0.0, 3.4)
    block_tier = jnp.broadcast_to(block_tier, (GROUP_SEQUENCES, block_count, POS_DEV, HEADS)).reshape(GROUP_SEQUENCES, PROMPT_LENGTH, HEADS)
    coarse_portion = jnp.clip(0.25 * jax.random.normal(key_b, (GROUP_SEQUENCES, PROMPT_LENGTH, HEADS), jnp.float32), -0.5, 0.5)
    spike_places = jax.random.randint(third_random_key, (GROUP_SEQUENCES, 3), 0, PROMPT_LENGTH)
    spike_mask = jnp.any(jnp.arange(PROMPT_LENGTH)[None, :, None] == spike_places[:, None, :], axis=-1)
    spike_length = jax.random.uniform(fourth_random_key, (GROUP_SEQUENCES, PROMPT_LENGTH, 1), jnp.float32, 7.5, 9.0)
    grand_sum = block_tier + coarse_portion + jnp.where(spike_mask[:, :, None], spike_length, 0.0)
    return grand_sum.astype(jnp.bfloat16)


def levels(stream_key, shape, shards, smallest, high):
    factor_of = 1.0
    for dim, parts in shards:
        heights = jax.random.uniform(jax.random.fold_in(jax.random.fold_in(stream_key, 6), dim), (parts,), jnp.float32, smallest / len(shards), high / len(shards))
        factor_of = factor_of * jnp.repeat(jnp.exp(heights), shape[dim] // parts).reshape((-1,) + (1,) * (len(shape) - 1 - dim))
    return factor_of


def scatter_about(own_key, dims, scale, reach, pieces=(), kind=jnp.bfloat16):
    result = jax.random.normal(own_key, dims, jnp.float32) * scale
    if len(pieces) > 0:
        result = levels(own_key, dims, pieces, -0.22, 0.18) * result
    return jnp.clip(result, min=-reach, max=reach).astype(kind)


def setup_inputs(seed: int = 0, part: int = 0) -> dict:
    arg_keys = jax.random.split(jax.random.key(seed), 7)
    part_splits = jax.random.split(jax.random.fold_in(arg_keys[6], part), 7)
    return {
        "tokens": scatter_about(part_splits[0], (GROUP_SEQUENCES, PROMPT_LENGTH, D), 1.0, 6.0, ((1, 256),)),
        "key_weight": scatter_about(arg_keys[1], (D, HEADS * HEAD_DIM), D ** -0.5, 0.125, ((0, 32),)),
        "value_weight": scatter_about(arg_keys[2], (D, HEADS * HEAD_DIM), D ** -0.5, 0.125, ((0, 32),)),
        "queries": scatter_about(part_splits[3], (GROUP_SEQUENCES, HEADS * HEAD_DIM), 1.0, 6.0),
        "head_offset": draw_head_offset(jax.random.fold_in(arg_keys[6], 71), part),
        "key_bias": draw_key_bias(jax.random.fold_in(jax.random.fold_in(arg_keys[6], part), 71), part),
    }


def reference(tokens, key_weight, value_weight, queries, head_offset, key_bias):
    score_scale = HEAD_DIM ** (-0.5)

    def one_sequence(inputs):
        tok_rows, key_offsets, query_row = inputs
        key_rows = jnp.dot(tok_rows, key_weight, preferred_element_type=jnp.float32).astype(jnp.bfloat16)
        value_rows = jnp.dot(tok_rows, value_weight, preferred_element_type=jnp.float32).astype(jnp.bfloat16)
        key_heads = key_rows.reshape(PROMPT_LENGTH, HEADS, HEAD_DIM).astype(jnp.float32)
        value_heads = value_rows.reshape(PROMPT_LENGTH, HEADS, HEAD_DIM).astype(jnp.float32)
        query_heads = query_row.reshape(HEADS, HEAD_DIM).astype(jnp.float32)
        logits = jnp.einsum('thc,hc->ht', key_heads, query_heads) * score_scale
        logits = logits + head_offset[:, None] + key_offsets.astype(jnp.float32).T
        fading = jax.nn.log_sigmoid(-logits)
        beyond = lax.cumsum(fading, axis=1, reverse=True) - fading
        weights = jnp.exp(jax.nn.log_sigmoid(logits) + beyond).astype(jnp.bfloat16)
        mixture = jnp.einsum('ht,thc->hc', weights.astype(jnp.float32), value_heads)
        normed = mixture * lax.rsqrt(lax.optimization_barrier(jnp.mean(mixture * mixture, axis=1, keepdims=True)) + 1e-06)
        return (key_rows, value_rows, normed.reshape(HEADS * HEAD_DIM))
    key_rows, value_rows, reading = lax.map(one_sequence, (tokens, key_bias, queries))
    return (key_rows, value_rows, key_bias, reading)
```

```python
import functools

import jax
import jax.numpy as jnp
from jax import lax
from jax.experimental import pallas as pl
from jax.experimental.pallas import tpu as pltpu
from jax.sharding import PartitionSpec as P

MESH = pl.DeviceIdType.MESH
CHUNKS = 8
EARLY = 4


def strictly_later(size):
    row = lax.broadcasted_iota(jnp.int32, (size, size), 0)
    col = lax.broadcasted_iota(jnp.int32, (size, size), 1)
    return jnp.where(row > col, 1.0, 0.0).astype(jnp.float32)


def kernel(
    tok_ref, kw_ref, vw_ref, q_ref, off_ref, bias_ref,
    key_out, value_out, bias_out, read_out,
    tbuf, wa, wb, kv, bb, bsel, part, r1, mid, r2, rd,
    load_sem, t_send, t_recv, s_send, s_recv, b_send, b_recv,
    ay_send, ay_recv, az_send, az_recv, bz_send, bz_recv, by_send, by_recv,
    o_send, o_recv, st_sem, f1_send, f1_recv, f2_send, f2_recv, hello,
):
    gr, sp, tp = lax.axis_index("gr"), lax.axis_index("sp"), lax.axis_index("tp")
    zl, y = sp // 4, sp % 4
    z = gr * 8 + zl
    x, c = tp // 2, tp % 2
    px, ox = x + 1 - 2 * (x % 2), 3 - x
    half = x // 2
    ptp, otp, stp = px * 2 + c, ox * 2 + c, x * 2 + 1 - c
    dm = (x % 2) * 2 + c
    ds = (x % 2) * 2 + 1 - c
    dp = (1 - x % 2) * 2 + c
    dq = (1 - x % 2) * 2 + 1 - c

    def at_tp(t):
        return (gr, sp, t)

    def at_y(k):
        return (gr, zl * 4 + (y + k) % 4, tp)

    def at_z(k):
        there = (z + k + 16) % 16
        return (there // 8, (there % 8) * 4 + y, tp)

    def remote(src, dst, send, recv, device):
        return pltpu.make_async_remote_copy(
            src_ref=src, dst_ref=dst, send_sem=send, recv_sem=recv,
            device_id=device, device_id_type=MESH,
        )

    pending = []

    def push(*args):
        copy = remote(*args)
        copy.start()
        pending.append(copy)

    tok_load = pltpu.make_async_copy(tok_ref, tbuf.at[dm], load_sem.at[0])
    tok_load.start()
    own_rows = pl.ds(pl.multiple_of(sp * 64, 64), 64)
    loads = []
    for n, (w_ref, lane) in enumerate(((kw_ref, 0), (vw_ref, 128))):
        for m, (buf, t) in enumerate(((wa, tp), (wb, otp))):
            cols = pl.ds(pl.multiple_of(t * 128, 128), 128)
            load = pltpu.make_async_copy(
                w_ref.at[:, cols], buf.at[own_rows, pl.ds(lane, 128)],
                load_sem.at[1 + n * 2 + m],
            )
            load.start()
            loads.append(load)
    bias_load = pltpu.make_async_copy(bias_ref, bb.at[tp], load_sem.at[5])
    bias_load.start()

    barrier = pltpu.get_barrier_semaphore()
    greeted = [at_tp((tp + k) % 8) for k in range(1, 8)]
    greeted += [at_y(k) for k in range(1, 4)]
    greeted += [(gr, zl * 4 + (y + k) % 4, otp) for k in range(1, 4)]
    greeted += [at_z(1), at_z(-1)]
    for device in greeted:
        pl.semaphore_signal(barrier, inc=1, device_id=device, device_id_type=MESH)
    pl.semaphore_wait(barrier, len(greeted))

    rows_of = 256 // CHUNKS

    def t_copy(k):
        piece = (dm, pl.ds(k * rows_of, rows_of))
        return remote(tbuf.at[piece], tbuf.at[piece], t_send.at[k], t_recv.at[k], at_tp(ptp))

    def t_arrival(k):
        piece = (dp, pl.ds(k * rows_of, rows_of))
        return remote(tbuf.at[piece], tbuf.at[piece], t_send.at[k], t_recv.at[k], at_tp(ptp))

    def t_forward(k):
        piece = (dp, pl.ds(k * rows_of, rows_of))
        return remote(tbuf.at[piece], tbuf.at[piece], s_send.at[k], s_recv.at[k], at_tp(stp))

    def s_arrival(k):
        piece = (dq, pl.ds(k * rows_of, rows_of))
        return remote(tbuf.at[piece], tbuf.at[piece], s_send.at[k], s_recv.at[k], at_tp(stp))

    for load in loads:
        load.wait()
    for k in range(1, 4):
        push(wa.at[own_rows], wa.at[own_rows], ay_send.at[k - 1], ay_recv.at[k - 1], at_y(k))

    def b_rows(offset, start=0, size=64):
        block = (zl + offset + 8) % 8
        return pl.ds(pl.multiple_of(block * 256 + y * 64 + start, 32), size)

    def b_rows_from(k, offset):
        block = (zl + offset + 8) % 8
        return pl.ds(pl.multiple_of(block * 256 + ((y - k + 4) % 4) * 64, 64), 64)

    def a_rows(offset, start=0, size=256):
        block = (zl + offset + 8) % 8
        return pl.ds(pl.multiple_of(block * 256 + start, 128), size)

    def b_spread(q, offset):
        for k in range(1, 4):
            n = q * 3 + k - 1
            push(wb.at[b_rows(offset)], wb.at[b_rows(offset)], by_send.at[n], by_recv.at[n], at_y(k))

    def b_z(side, j):
        sign = 1 if side == 0 else -1
        if j < 4:
            rows = b_rows(-sign * (j - 1))
        else:
            rows = b_rows(-sign * 3, 32 * side, 32)
        n = side * 4 + j - 1
        push(wb.at[rows], wb.at[rows], bz_send.at[n], bz_recv.at[n], at_z(sign))

    def b_z_wait(side, j):
        sign = 1 if side == 0 else -1
        rows = b_rows(-sign * j) if j < 4 else b_rows(4, 32 * side, 32)
        n = side * 4 + j - 1
        remote(wb.at[rows], wb.at[rows], bz_send.at[n], bz_recv.at[n], at_z(sign)).wait_recv()

    def a_z(side, j):
        sign = 1 if side == 0 else -1
        if j < 4:
            rows = a_rows(-sign * (j - 1))
        else:
            rows = a_rows(-sign * 3, 128 * side, 128)
        n = side * 4 + j - 1
        push(wa.at[rows], wa.at[rows], az_send.at[n], az_recv.at[n], at_z(sign))

    def a_z_wait(side, j):
        sign = 1 if side == 0 else -1
        rows = a_rows(-sign * j) if j < 4 else a_rows(4, 128 * side, 128)
        n = side * 4 + j - 1
        remote(wa.at[rows], wa.at[rows], az_send.at[n], az_recv.at[n], at_z(sign)).wait_recv()

    b_z(0, 1)
    b_z(1, 1)
    tok_load.wait()
    for k in range(CHUNKS):
        copy = t_copy(k)
        copy.start()
        pending.append(copy)
    push(tbuf.at[dm], tbuf.at[dm], s_send.at[CHUNKS], s_recv.at[CHUNKS], at_tp(stp))
    b_spread(0, 0)
    bias_load.wait()
    for k in range(1, 8):
        push(bb.at[tp], bb.at[tp], b_send.at[k - 1], b_recv.at[k - 1], at_tp((tp + k) % 8))

    for k in range(1, 4):
        rows = pl.ds(pl.multiple_of(zl * 256 + ((y - k + 4) % 4) * 64, 64), 64)
        remote(wa.at[rows], wa.at[rows], ay_send.at[k - 1], ay_recv.at[k - 1], at_y(k)).wait_recv()
    a_z(0, 1)
    a_z(1, 1)

    def b_step(j):
        for side in (0, 1):
            b_z_wait(side, j)
            if j < 4:
                b_z(side, j + 1)
                b_spread(2 * j - 1 + side, -j if side == 0 else j)
        if j == 4:
            b_spread(7, 4)

    def a_step(j):
        for side in (0, 1):
            a_z_wait(side, j)
            if j < 4:
                a_z(side, j + 1)

    def forward_step(k):
        t_arrival(k).wait_recv()
        copy = t_forward(k)
        copy.start()
        pending.append(copy)

    b_step(1)
    b_step(2)
    a_step(1)
    forward_step(0)
    b_step(3)
    a_step(2)
    forward_step(1)
    b_step(4)
    a_step(3)
    forward_step(2)
    a_step(4)
    forward_step(3)
    offsets = (0, -1, 1, -2, 2, -3, 3, 4)
    for q in range(8):
        for k in range(1, 4):
            n = q * 3 + k - 1
            rows = b_rows_from(k, offsets[q])
            remote(wb.at[rows], wb.at[rows], by_send.at[n], by_recv.at[n], at_y(k)).wait_recv()

    def project(tokens, s, d, first, count):
        for g, w in enumerate((wa, wb)):
            out = jnp.dot(tokens, w[...], preferred_element_type=jnp.float32).astype(jnp.bfloat16)
            for n in range(len(d)):
                rows = out[n * count : (n + 1) * count]
                kv[g, 0, s, d[n], pl.ds(first, count), :] = rows[:, :128]
                kv[g, 1, s, d[n], pl.ds(first, count), :] = rows[:, 128:]

    outs = (key_out, value_out)

    def o_copy(s, d, v, where):
        n = d * 4 + s * 2 + v
        return remote(
            kv.at[1, v, s, d], outs[v].at[s, where, d], o_send.at[n], o_recv.at[n], at_tp(otp)
        )

    def send_out(s, d):
        for v in (0, 1):
            o_copy(s, d, v, half).start()

    remote(tbuf.at[ds], tbuf.at[ds], s_send.at[CHUNKS], s_recv.at[CHUNKS], at_tp(stp)).wait_recv()

    def early(n, carry):
        s, which = n % 2, n // 2
        d = jnp.where(which == 0, dm, ds)
        project(tbuf[d, pl.ds(pl.multiple_of(s * 128, 128), 128), :], s, (d,), 0, 128)
        send_out(s, d)
        return carry

    lax.fori_loop(0, 4, early, 0)
    for k in range(EARLY):
        s_arrival(k).wait_recv()

    def early_partner(n, carry):
        d = jnp.where(n == 0, dp, dq)
        project(tbuf[d, pl.ds(0, 128), :], 0, (d,), 0, 128)
        send_out(0, d)
        return carry

    lax.fori_loop(0, 2, early_partner, 0)

    def up():
        @pl.when(zl > 0)
        def _():
            pl.semaphore_wait(hello.at[0], 1)

        @pl.when(zl < 7)
        def _():
            pl.semaphore_signal(hello.at[0], inc=1, device_id=at_z(1), device_id_type=MESH)

    def down():
        @pl.when(zl < 7)
        def _():
            pl.semaphore_wait(hello.at[1], 1)

        @pl.when(zl > 0)
        def _():
            pl.semaphore_signal(hello.at[1], inc=1, device_id=at_z(-1), device_id_type=MESH)

    @pl.when(zl < 4)
    def _():
        up()
        down()

    @pl.when(zl >= 4)
    def _():
        down()
        up()

    def late(k, carry):
        t_arrival(k).wait_recv()
        t_forward(k).start()
        s_arrival(k).wait_recv()
        first = pl.multiple_of((k - EARLY) * rows_of, rows_of)
        here = pl.ds(pl.multiple_of(k * rows_of, rows_of), rows_of)
        both = jnp.concatenate([tbuf[dp, here, :], tbuf[dq, here, :]], axis=0)
        project(both, 1, (dp, dq), first, rows_of)
        return carry

    lax.fori_loop(EARLY, CHUNKS, late, 0)
    send_out(1, dp)
    send_out(1, dq)

    stores = []
    for v in (0, 1):
        for s in (0, 1):
            store = pltpu.make_async_copy(kv.at[0, v, s], outs[v].at[s, half], st_sem.at[v * 2 + s])
            store.start()
            stores.append(store)

    for k in range(1, 8):
        src = (tp - k + 8) % 8
        remote(bb.at[src], bb.at[src], b_send.at[k - 1], b_recv.at[k - 1], at_tp(src)).wait_recv()
    row = lax.broadcasted_iota(jnp.int32, (8, 32), 0)
    col = lax.broadcasted_iota(jnp.int32, (8, 32), 1)
    group_tp = jnp.where(row < 4, tp, otp)
    wanted = ((row // 2) % 2) * 16 + group_tp * 2 + row % 2
    select = jnp.where(col == wanted, 1.0, 0.0).astype(jnp.bfloat16)
    for d in range(8):
        picked = jnp.dot(select, bb[d].reshape(32, 128), preferred_element_type=jnp.float32)
        bsel[d] = picked
        for s in (0, 1):
            bias_out_rows = picked[2 * s : 2 * s + 2].astype(jnp.bfloat16)
            rd_rows = pl.ds(d * 128, 128)
            part_bias(bias_out, s, rd_rows, bias_out_rows)

    lane = lax.broadcasted_iota(jnp.int32, (8, 128), 1)
    row8 = lax.broadcasted_iota(jnp.int32, (8, 128), 0)
    own_lane = (lane // 64) == (row8 % 2)
    hrow = lax.broadcasted_iota(jnp.int32, (8, 16), 0)
    hcol = lax.broadcasted_iota(jnp.int32, (8, 16), 1)
    head = jnp.where(hrow < 4, tp, otp) * 2 + hrow % 2
    offset = jnp.sum(
        jnp.where(hcol == head, jnp.broadcast_to(off_ref[...], (8, 16)), 0.0), axis=1, keepdims=True
    )
    queries = []
    for g, t in enumerate((tp, otp)):
        cols = q_ref[:, pl.ds(pl.multiple_of(t * 128, 128), 128)].astype(jnp.float32)
        for s in (0, 1):
            mine = own_lane & (row8 // 2 == g * 2 + s)
            spread = jnp.broadcast_to(cols[s : s + 1], (8, 128))
            queries.append(jnp.where(mine, spread, 0.0).astype(jnp.bfloat16))
    later = strictly_later(128)
    ls, within, totals = [], [], []
    for d in range(4):
        score = jnp.zeros((8, 128), jnp.float32)
        for g in (0, 1):
            for s in (0, 1):
                score += lax.dot_general(
                    queries[g * 2 + s], kv[g, 0, s, d], (((1,), (1,)), ((), ())),
                    preferred_element_type=jnp.float32,
                )
        logit = score * 0.125 + offset + bsel[half * 4 + d]
        tail = jnp.log1p(jnp.exp(-jnp.abs(logit)))
        fading = -(jnp.maximum(logit, 0.0) + tail)
        ls.append(jnp.minimum(logit, 0.0) - tail)
        within.append(
            jnp.dot(fading, later, precision=lax.Precision.HIGHEST, preferred_element_type=jnp.float32)
        )
        totals.append(jnp.sum(fading, axis=1, keepdims=True))
    carried = jnp.zeros((8, 1), jnp.float32)
    mixture = jnp.zeros((8, 128), jnp.float32)
    for d in (3, 2, 1, 0):
        weight = jnp.exp(ls[d] + within[d] + carried)
        carried = carried + totals[d]
        high = weight.astype(jnp.bfloat16)
        low = (weight - high.astype(jnp.float32)).astype(jnp.bfloat16)
        for g in (0, 1):
            for s in (0, 1):
                values = kv[g, 1, s, d]
                product = jnp.dot(high, values, preferred_element_type=jnp.float32)
                product += jnp.dot(low, values, preferred_element_type=jnp.float32)
                mixture += jnp.where(row8 // 2 == g * 2 + s, product, 0.0)
    mixture = jnp.where(own_lane, mixture, 0.0)
    sums = jnp.where(own_lane, jnp.broadcast_to(carried, (8, 128)), 0.0)
    for g in (0, 1):
        lines = []
        for block in (mixture, sums):
            for s in (0, 1):
                r = g * 4 + s * 2
                lines.append(block[r : r + 1] + block[r + 1 : r + 2])
        part[g] = jnp.concatenate(lines, axis=0)

    def f1(slot, device, g):
        return remote(part.at[g], r1.at[slot], f1_send.at[g * 4 + slot // 2], f1_recv.at[slot], device)

    mine = y * 2 + half
    firsts = []
    for k in range(1, 4):
        copy = remote(part.at[0], r1.at[mine], f1_send.at[k], f1_recv.at[mine], at_y(k))
        copy.start()
        firsts.append(copy)
    for k in range(0, 4):
        device = (gr, zl * 4 + (y + k) % 4, otp)
        copy = remote(part.at[1], r1.at[mine], f1_send.at[4 + k], f1_recv.at[mine], device)
        copy.start()
        firsts.append(copy)
    own = pltpu.make_async_copy(part.at[0], r1.at[mine], f1_send.at[0])
    own.start()
    own.wait()
    for k in range(1, 4):
        slot = ((y + k) % 4) * 2 + half
        remote(part.at[0], r1.at[slot], f1_send.at[k], f1_recv.at[slot], at_y(k)).wait_recv()
    for k in range(0, 4):
        slot = ((y + k) % 4) * 2 + 1 - half
        remote(part.at[1], r1.at[slot], f1_send.at[4 + k], f1_recv.at[slot], at_tp(otp)).wait_recv()

    def combine(buf):
        total = buf[7][2:4]
        mixed = buf[7][0:2]
        for n in range(6, -1, -1):
            block = buf[n]
            mixed = mixed + block[0:2] * jnp.exp(total)
            total = total + block[2:4]
        return mixed, total

    mixed, total = combine(r1)
    mid[...] = jnp.concatenate([mixed, total], axis=0)
    seconds = []
    for k in range(1, 8):
        device = (gr, ((zl + k) % 8) * 4 + y, tp)
        copy = remote(mid, r2.at[zl], f2_send.at[k], f2_recv.at[zl], device)
        copy.start()
        seconds.append(copy)
    own = pltpu.make_async_copy(mid, r2.at[zl], f2_send.at[0])
    own.start()
    own.wait()
    for k in range(1, 8):
        slot = (zl + k) % 8
        remote(mid, r2.at[slot], f2_send.at[k], f2_recv.at[slot], at_z(1)).wait_recv()
    mixed, total = combine(r2)
    square = mixed * mixed
    first_head = lax.broadcasted_iota(jnp.int32, (2, 128), 1) < 64
    mean_a = jnp.sum(jnp.where(first_head, square, 0.0), axis=1, keepdims=True) * (1.0 / 64)
    mean_b = jnp.sum(jnp.where(first_head, 0.0, square), axis=1, keepdims=True) * (1.0 / 64)
    read_out[...] = mixed * lax.rsqrt(jnp.where(first_head, mean_a, mean_b) + 1e-06)

    for copy in pending + firsts + seconds:
        copy.wait_send()

    def forwarded(k, carry):
        t_forward(k).wait_send()
        return carry

    lax.fori_loop(EARLY, CHUNKS, forwarded, 0)

    def sent(n, carry):
        s, d = n % 2, n // 2
        for v in (0, 1):
            copy = o_copy(s, d, v, half)
            copy.wait_send()
            o_copy(s, d, v, 1 - half).wait_recv()
        return carry

    lax.fori_loop(0, 8, sent, 0)
    for store in stores:
        store.wait()


def part_bias(bias_out, s, cols, rows):
    bias_out[s, :, cols] = rows


def per_device(tokens, key_weight, value_weight, queries, head_offset, key_bias):
    any_space = pl.BlockSpec(memory_space=pl.ANY)
    vmem = pl.BlockSpec(memory_space=pltpu.VMEM)
    dma = pltpu.SemaphoreType.DMA
    cache = jax.ShapeDtypeStruct((2, 2, 4, 128, 128), jnp.bfloat16)
    keys, values, bias, reading = pl.pallas_call(
        kernel,
        out_shape=(
            cache,
            cache,
            jax.ShapeDtypeStruct((2, 2, 1024), jnp.bfloat16),
            jax.ShapeDtypeStruct((2, 128), jnp.float32),
        ),
        in_specs=[any_space, any_space, any_space, vmem, vmem, any_space],
        out_specs=(any_space, any_space, vmem, vmem),
        scratch_shapes=[
            pltpu.VMEM((4, 256, 2048), jnp.bfloat16),
            pltpu.VMEM((2048, 256), jnp.bfloat16),
            pltpu.VMEM((2048, 256), jnp.bfloat16),
            pltpu.VMEM((2, 2, 2, 4, 128, 128), jnp.bfloat16),
            pltpu.VMEM((8, 2, 16, 128), jnp.bfloat16),
            pltpu.VMEM((8, 8, 128), jnp.float32),
            pltpu.VMEM((2, 4, 128), jnp.float32),
            pltpu.VMEM((8, 4, 128), jnp.float32),
            pltpu.VMEM((4, 128), jnp.float32),
            pltpu.VMEM((8, 4, 128), jnp.float32),
            pltpu.VMEM((2, 128), jnp.float32),
            dma((6,)),
            dma((CHUNKS,)), dma((CHUNKS,)), dma((CHUNKS + 1,)), dma((CHUNKS + 1,)),
            dma((7,)), dma((7,)),
            dma((3,)), dma((3,)), dma((8,)), dma((8,)), dma((8,)), dma((8,)),
            dma((24,)), dma((24,)),
            dma((16,)), dma((16,)), dma((4,)),
            dma((8,)), dma((8,)), dma((8,)), dma((8,)),
            pltpu.SemaphoreType.REGULAR((2,)),
        ],
        name="prefill",
        compiler_params=pltpu.CompilerParams(collective_id=0, has_side_effects=True),
    )(
        tokens.reshape(256, 2048),
        key_weight,
        value_weight,
        queries,
        head_offset.reshape(1, 16),
        jnp.transpose(key_bias, (0, 2, 1)),
    )
    return (
        keys.reshape(2, 1024, 128),
        values.reshape(2, 1024, 128),
        jnp.transpose(bias, (0, 2, 1)),
        reading,
    )


def solution(mesh):
    placed = (
        P("gr", ("sp", "tp"), None),
        P("sp", None),
        P("sp", None),
        P("gr", None),
        P(),
        P("gr", ("sp", "tp"), None),
    )
    return jax.shard_map(
        per_device,
        mesh=mesh,
        in_specs=placed,
        out_specs=(P("gr", "sp", "tp"), P("gr", "sp", "tp"), P("gr", "sp", "tp"), P("gr", "tp")),
        check_vma=False,
    )
```

```python
import functools

import jax
import jax.numpy as jnp
from jax import lax
from jax.experimental import pallas as pl
from jax.experimental.pallas import tpu as pltpu
from jax.sharding import PartitionSpec as P

MESH = pl.DeviceIdType.MESH
CHUNKS = 8
EARLY = 4


def strictly_later(size):
    row = lax.broadcasted_iota(jnp.int32, (size, size), 0)
    col = lax.broadcasted_iota(jnp.int32, (size, size), 1)
    return jnp.where(row > col, 1.0, 0.0).astype(jnp.float32)


def kernel(
    tok_ref, kw_ref, vw_ref, q_hbm, off_hbm, bias_ref,
    cache_out, bias_out, read_out,
    tbuf, wa, wb, kv, bb, bsel, part, r1, mid, r2, q_ref, off_ref,
    load_sem, t_send, t_recv, s_send, s_recv, b_send, b_recv,
    ay_send, ay_recv, z_send, z_recv, by_send, by_recv,
    o_send, o_recv, f1_send, f1_recv, f2_send, f2_recv, hello,
):
    gr, sp, tp = lax.axis_index("gr"), lax.axis_index("sp"), lax.axis_index("tp")
    zl, y = sp // 4, sp % 4
    z = gr * 8 + zl
    x, c = tp // 2, tp % 2
    px, ox = x + 1 - 2 * (x % 2), 3 - x
    half = x // 2
    ptp, otp, stp = px * 2 + c, ox * 2 + c, x * 2 + 1 - c
    dm = (x % 2) * 2 + c
    ds = (x % 2) * 2 + 1 - c
    dp = (1 - x % 2) * 2 + c
    dq = (1 - x % 2) * 2 + 1 - c

    def at_tp(t):
        return (gr, sp, t)

    def at_y(k):
        return (gr, zl * 4 + (y + k) % 4, tp)

    def at_z(k):
        there = (z + k + 16) % 16
        return (there // 8, (there % 8) * 4 + y, tp)

    def remote(src, dst, send, recv, device):
        return pltpu.make_async_remote_copy(
            src_ref=src, dst_ref=dst, send_sem=send, recv_sem=recv,
            device_id=device, device_id_type=MESH,
        )

    pending = []

    def push(*args):
        copy = remote(*args)
        copy.start()
        pending.append(copy)

    tok_load = pltpu.make_async_copy(tok_ref, tbuf.at[dm], load_sem.at[0])
    tok_load.start()
    own_rows = pl.ds(pl.multiple_of(sp * 64, 64), 64)
    loads = []
    for n, (w_ref, lane) in enumerate(((kw_ref, 0), (vw_ref, 128))):
        for m, (buf, t) in enumerate(((wa, tp), (wb, otp))):
            cols = pl.ds(pl.multiple_of(t * 128, 128), 128)
            load = pltpu.make_async_copy(
                w_ref.at[:, cols], buf.at[own_rows, pl.ds(lane, 128)],
                load_sem.at[1 + n * 2 + m],
            )
            load.start()
            loads.append(load)
    bias_load = pltpu.make_async_copy(bias_ref, bb.at[tp], load_sem.at[5])
    bias_load.start()
    q_load = pltpu.make_async_copy(q_hbm, q_ref, load_sem.at[6])
    q_load.start()
    off_load = pltpu.make_async_copy(off_hbm, off_ref, load_sem.at[7])
    off_load.start()

    barrier = pltpu.get_barrier_semaphore()
    lowest, highest = z == 0, z == 15

    def greet(device):
        pl.semaphore_signal(barrier, inc=1, device_id=device, device_id_type=MESH)

    for k in (2, 1, 3):
        greet(at_y(k))
    for k in range(1, 8):
        greet(at_tp((tp + k) % 8))

    @pl.when(jnp.logical_not(highest))
    def _():
        greet(at_z(1))

    @pl.when(jnp.logical_not(lowest))
    def _():
        greet(at_z(-1))
        pl.semaphore_wait(barrier, 12)

    @pl.when(lowest)
    def _():
        pl.semaphore_wait(barrier, 11)
        greet(at_z(-1))

    @pl.when(highest)
    def _():
        greet(at_z(1))

    rows_of = 256 // CHUNKS

    def t_copy(k):
        piece = (dm, pl.ds(k * rows_of, rows_of))
        return remote(tbuf.at[piece], tbuf.at[piece], t_send.at[k], t_recv.at[k], at_tp(ptp))

    def t_arrival(k):
        piece = (dp, pl.ds(k * rows_of, rows_of))
        return remote(tbuf.at[piece], tbuf.at[piece], t_send.at[k], t_recv.at[k], at_tp(ptp))

    def t_forward(k):
        piece = (dp, pl.ds(k * rows_of, rows_of))
        return remote(tbuf.at[piece], tbuf.at[piece], s_send.at[k], s_recv.at[k], at_tp(stp))

    def s_arrival(k):
        piece = (dq, pl.ds(k * rows_of, rows_of))
        return remote(tbuf.at[piece], tbuf.at[piece], s_send.at[k], s_recv.at[k], at_tp(stp))

    def forward_step(k):
        t_arrival(k).wait_recv()
        copy = t_forward(k)
        copy.start()
        pending.append(copy)

    tok_load.wait()
    for k in range(CHUNKS):
        copy = t_copy(k)
        copy.start()
        pending.append(copy)
    push(tbuf.at[dm], tbuf.at[dm], s_send.at[CHUNKS], s_recv.at[CHUNKS], at_tp(stp))

    shifts = (0, 0, 1, 3, 2)

    def rows_at(offset, shift, start=0, size=64):
        block = (zl + offset + 8) % 8
        return pl.ds(pl.multiple_of(block * 256 + ((y - shift + 4) % 4) * 64 + start, 32), size)

    def z_piece(p, offset, start=0, size=64):
        return (wb if p == 0 else wa).at[rows_at(offset, shifts[p], start, size)]

    def z_push(side, p, j):
        sign = 1 if side == 0 else -1
        if j < 4:
            piece = z_piece(p, -sign * (j - 1))
        else:
            piece = z_piece(p, -sign * 3, 32 * side, 32)
        n = (side * 5 + p) * 4 + j - 1
        push(piece, piece, z_send.at[n], z_recv.at[n], at_z(sign))

    def z_wait(side, p, j):
        sign = 1 if side == 0 else -1
        piece = z_piece(p, -sign * j) if j < 4 else z_piece(p, 4, 32 * side, 32)
        n = (side * 5 + p) * 4 + j - 1
        remote(piece, piece, z_send.at[n], z_recv.at[n], at_z(sign)).wait_recv()

    def b_spread(q, offset):
        piece = wb.at[rows_at(offset, 0)]
        for k in (2, 1, 3):
            n = q * 3 + k - 1
            push(piece, piece, by_send.at[n], by_recv.at[n], at_y(k))

    for load in loads:
        load.wait()
    for k in (2, 1, 3):
        piece = wa.at[own_rows]
        push(piece, piece, ay_send.at[k - 1], ay_recv.at[k - 1], at_y(k))
    z_push(0, 0, 1)
    z_push(0, 1, 1)
    b_spread(0, 0)

    @pl.when(lowest)
    def _():
        pl.semaphore_wait(barrier, 1)

    z_push(1, 0, 1)
    z_push(1, 1, 1)
    bias_load.wait()
    for k in range(1, 8):
        push(bb.at[tp], bb.at[tp], b_send.at[k - 1], b_recv.at[k - 1], at_tp((tp + k) % 8))

    def z_step(p, j):
        for side in (0, 1):
            z_wait(side, p, j)
            if j < 4:
                z_push(side, p, j + 1)
                if p == 0:
                    b_spread(2 * j - 1 + side, -j if side == 0 else j)
        if j == 4 and p == 0:
            b_spread(7, 4)

    for p in (2, 3, 4):
        piece = wa.at[rows_at(0, shifts[p])]
        k = shifts[p]
        remote(piece, piece, ay_send.at[k - 1], ay_recv.at[k - 1], at_y(k)).wait_recv()
        z_push(0, p, 1)
        z_push(1, p, 1)
    for j in range(1, 5):
        for p in range(5):
            z_step(p, j)
        forward_step(j - 1)
    offsets = (0, -1, 1, -2, 2, -3, 3, 4)
    for q in range(8):
        for k in (1, 3, 2):
            n = q * 3 + k - 1
            piece = wb.at[rows_at(offsets[q], k)]
            remote(piece, piece, by_send.at[n], by_recv.at[n], at_y(k)).wait_recv()

    pl.semaphore_signal(hello.at[0], inc=1, device_id=at_tp(otp), device_id_type=MESH)

    @pl.when((zl >= 2) & (zl <= 4))
    def _():
        pl.semaphore_signal(hello.at[1], inc=1, device_id=at_z(3), device_id_type=MESH)

    @pl.when((zl >= 3) & (zl <= 5))
    def _():
        pl.semaphore_signal(hello.at[1], inc=1, device_id=at_z(-3), device_id_type=MESH)

    def project(tokens, s, d, first, count):
        for g, w in enumerate((wa, wb)):
            out = jnp.dot(tokens, w[...], preferred_element_type=jnp.float32).astype(jnp.bfloat16)
            for n in range(len(d)):
                for v in (0, 1):
                    block = out[n * count : (n + 1) * count, v * 128 : (v + 1) * 128]
                    if g == 0:
                        cache_out[v, s, half, d[n], pl.ds(first, count), :] = block
                    else:
                        kv[v, s, d[n], pl.ds(first, count), :] = block

    def o_copy(s, d, v, where):
        n = d * 4 + s * 2 + v
        return remote(
            kv.at[v, s, d], cache_out.at[v, s, where, d], o_send.at[n], o_recv.at[n], at_tp(otp)
        )

    def send_out(s, d):
        for v in (0, 1):
            o_copy(s, d, v, half).start()

    with jax.named_scope("sib"):
        remote(tbuf.at[ds], tbuf.at[ds], s_send.at[CHUNKS], s_recv.at[CHUNKS], at_tp(stp)).wait_recv()

    def early(n, carry):
        s, which = n % 2, n // 2
        d = jnp.where(which == 0, dm, ds)
        project(tbuf[d, pl.ds(pl.multiple_of(s * 128, 128), 128), :], s, (d,), 0, 128)
        send_out(s, d)
        return carry

    lax.fori_loop(0, 4, early, 0)
    for k in range(EARLY):
        s_arrival(k).wait_recv()

    def early_partner(n, carry):
        d = jnp.where(n == 0, dp, dq)
        project(tbuf[d, pl.ds(0, 128), :], 0, (d,), 0, 128)
        send_out(0, d)
        return carry

    lax.fori_loop(0, 2, early_partner, 0)
    forward_step(4)
    forward_step(5)

    q_load.wait()
    off_load.wait()
    for k in range(1, 8):
        src = (tp - k + 8) % 8
        remote(bb.at[src], bb.at[src], b_send.at[k - 1], b_recv.at[k - 1], at_tp(src)).wait_recv()
    row = lax.broadcasted_iota(jnp.int32, (8, 16), 0)
    col = lax.broadcasted_iota(jnp.int32, (8, 16), 1)
    head = jnp.where(row < 2, tp, otp) * 2 + row % 2
    chosen = (col == head) & (row < 4)
    select = jnp.where(chosen, 1.0, 0.0).astype(jnp.bfloat16)
    offset = jnp.sum(
        jnp.where(chosen, jnp.broadcast_to(off_ref[...], (8, 16)), 0.0), axis=1, keepdims=True
    )
    for d in range(8):
        for s in (0, 1):
            picked = jnp.dot(select, bb[d, s], preferred_element_type=jnp.float32)
            bsel[d, s] = picked
            bias_out[s, :, d * 128 : (d + 1) * 128] = picked[0:2].astype(jnp.bfloat16)
    lane = lax.broadcasted_iota(jnp.int32, (8, 128), 1)
    row8 = lax.broadcasted_iota(jnp.int32, (8, 128), 0)
    own_lane = (lane // 64) == (row8 % 2)

    def attend(s):
        score = jnp.zeros((8, 512), jnp.float32)
        for g, t in enumerate((tp, otp)):
            cols = q_ref[:, pl.ds(pl.multiple_of(t * 128, 128), 128)].astype(jnp.float32)
            spread = jnp.broadcast_to(cols[s : s + 1], (8, 128))
            query = jnp.where(own_lane & (row8 // 2 == g), spread, 0.0).astype(jnp.bfloat16)
            keys = cache_out[0, s, half] if g == 0 else kv[0, s]
            score += lax.dot_general(
                query, keys.reshape(512, 128), (((1,), (1,)), ((), ())),
                preferred_element_type=jnp.float32,
            )
        bias = jnp.concatenate([bsel[half * 4 + d, s] for d in range(4)], axis=1)
        logit = score * 0.125 + offset + bias
        tail = jnp.log1p(jnp.exp(-jnp.abs(logit)))
        fading = -(jnp.maximum(logit, 0.0) + tail)
        ls = jnp.minimum(logit, 0.0) - tail
        blocks = [fading[:, d * 128 : (d + 1) * 128] for d in range(4)]
        within = jnp.dot(
            jnp.concatenate(blocks, axis=0), strictly_later(128),
            precision=lax.Precision.HIGHEST, preferred_element_type=jnp.float32,
        )
        carried = jnp.zeros((8, 1), jnp.float32)
        beyond = [None] * 4
        for d in (3, 2, 1, 0):
            beyond[d] = within[d * 8 : d * 8 + 8] + carried
            carried = carried + jnp.sum(blocks[d], axis=1, keepdims=True)
        weight = jnp.exp(ls + jnp.concatenate(beyond, axis=1))
        high = weight.astype(jnp.bfloat16)
        low = (weight - high.astype(jnp.float32)).astype(jnp.bfloat16)
        both = jnp.concatenate([high, low], axis=0)
        sums = jnp.where(own_lane, jnp.broadcast_to(carried, (8, 128)), 0.0)
        for g in (0, 1):
            values = cache_out[1, s, half] if g == 0 else kv[1, s]
            product = jnp.dot(both, values.reshape(512, 128), preferred_element_type=jnp.float32)
            mixture = jnp.where(own_lane, product[0:8] + product[8:16], 0.0)
            r = 2 * g
            part[g, s : s + 1, :] = mixture[r : r + 1] + mixture[r + 1 : r + 2]
            part[g, 2 + s : 3 + s, :] = sums[r : r + 1] + sums[r + 1 : r + 2]

    with jax.named_scope("att0"):
        attend(0)

    def late(k):
        s_arrival(k).wait_recv()
        here = pl.ds(k * rows_of, rows_of)
        both = jnp.concatenate([tbuf[dp, here, :], tbuf[dq, here, :]], axis=0)
        project(both, 1, (dp, dq), (k - EARLY) * rows_of, rows_of)

    for k in range(EARLY, CHUNKS):
        if k >= 6:
            forward_step(k)
        late(k)
    send_out(1, dp)
    send_out(1, dq)
    with jax.named_scope("att1"):
        attend(1)
    pl.semaphore_wait(hello.at[0], 1)

    @pl.when((zl <= 2) | (zl >= 5))
    def _():
        pl.semaphore_wait(hello.at[1], 1)

    mine = y * 2 + half
    firsts = []
    for k in range(1, 4):
        copy = remote(part.at[0], r1.at[mine], f1_send.at[k], f1_recv.at[mine], at_y(k))
        copy.start()
        firsts.append(copy)
    for k in range(0, 4):
        device = (gr, zl * 4 + (y + k) % 4, otp)
        copy = remote(part.at[1], r1.at[mine], f1_send.at[4 + k], f1_recv.at[mine], device)
        copy.start()
        firsts.append(copy)
    own = pltpu.make_async_copy(part.at[0], r1.at[mine], f1_send.at[0])
    own.start()
    own.wait()
    for k in range(1, 4):
        slot = ((y + k) % 4) * 2 + half
        remote(part.at[0], r1.at[slot], f1_send.at[k], f1_recv.at[slot], at_y(k)).wait_recv()
    for k in range(0, 4):
        slot = ((y + k) % 4) * 2 + 1 - half
        remote(part.at[1], r1.at[slot], f1_send.at[4 + k], f1_recv.at[slot], at_tp(otp)).wait_recv()

    def combine(buf):
        total = buf[7][2:4]
        mixed = buf[7][0:2]
        for n in range(6, -1, -1):
            block = buf[n]
            mixed = mixed + block[0:2] * jnp.exp(total)
            total = total + block[2:4]
        return mixed, total

    mixed, total = combine(r1)
    mid[...] = jnp.concatenate([mixed, total], axis=0)
    seconds = []
    for k in range(1, 8):
        device = (gr, ((zl + k) % 8) * 4 + y, tp)
        copy = remote(mid, r2.at[zl], f2_send.at[k], f2_recv.at[zl], device)
        copy.start()
        seconds.append(copy)
    own = pltpu.make_async_copy(mid, r2.at[zl], f2_send.at[0])
    own.start()
    own.wait()
    for k in range(1, 8):
        slot = (zl + k) % 8
        remote(mid, r2.at[slot], f2_send.at[k], f2_recv.at[slot], at_z(1)).wait_recv()
    mixed, total = combine(r2)
    square = mixed * mixed
    first_head = lax.broadcasted_iota(jnp.int32, (2, 128), 1) < 64
    mean_a = jnp.sum(jnp.where(first_head, square, 0.0), axis=1, keepdims=True) * (1.0 / 64)
    mean_b = jnp.sum(jnp.where(first_head, 0.0, square), axis=1, keepdims=True) * (1.0 / 64)
    read_out[...] = mixed * lax.rsqrt(jnp.where(first_head, mean_a, mean_b) + 1e-06)

    for copy in pending + firsts + seconds:
        copy.wait_send()

    def sent(n, carry):
        s, d = n % 2, n // 2
        for v in (0, 1):
            o_copy(s, d, v, half).wait_send()
            o_copy(s, d, v, 1 - half).wait_recv()
        return carry

    lax.fori_loop(0, 8, sent, 0)


def finish(cache_ref, bias_ref, read_ref, key_out, value_out, bias_out, read_out, sem):
    pairs = (
        (cache_ref.at[0], key_out), (cache_ref.at[1], value_out),
        (bias_ref, bias_out), (read_ref, read_out),
    )
    copies = [pltpu.make_async_copy(src, dst, sem.at[n]) for n, (src, dst) in enumerate(pairs)]
    for copy in copies:
        copy.start()
    for copy in copies:
        copy.wait()


def per_device(tokens, key_weight, value_weight, queries, head_offset, key_bias):
    any_space = pl.BlockSpec(memory_space=pl.ANY)
    vmem = pl.BlockSpec(memory_space=pltpu.VMEM)
    dma = pltpu.SemaphoreType.DMA
    held, bias, reading = pl.pallas_call(
        kernel,
        out_shape=(
            pltpu.VMEM((2, 2, 2, 4, 128, 128), jnp.bfloat16),
            pltpu.VMEM((2, 2, 1024), jnp.bfloat16),
            pltpu.VMEM((2, 128), jnp.float32),
        ),
        in_specs=[any_space] * 6,
        out_specs=(vmem, vmem, vmem),
        scratch_shapes=[
            pltpu.VMEM((4, 256, 2048), jnp.bfloat16),
            pltpu.VMEM((2048, 256), jnp.bfloat16),
            pltpu.VMEM((2048, 256), jnp.bfloat16),
            pltpu.VMEM((2, 2, 4, 128, 128), jnp.bfloat16),
            pltpu.VMEM((8, 2, 16, 128), jnp.bfloat16),
            pltpu.VMEM((8, 2, 8, 128), jnp.float32),
            pltpu.VMEM((2, 4, 128), jnp.float32),
            pltpu.VMEM((8, 4, 128), jnp.float32),
            pltpu.VMEM((4, 128), jnp.float32),
            pltpu.VMEM((8, 4, 128), jnp.float32),
            pltpu.VMEM((2, 1024), jnp.bfloat16),
            pltpu.VMEM((1, 16), jnp.float32),
            dma((8,)),
            dma((CHUNKS,)), dma((CHUNKS,)), dma((CHUNKS + 1,)), dma((CHUNKS + 1,)),
            dma((7,)), dma((7,)),
            dma((3,)), dma((3,)), dma((40,)), dma((40,)), dma((24,)), dma((24,)),
            dma((16,)), dma((16,)),
            dma((8,)), dma((8,)), dma((8,)), dma((8,)),
            pltpu.SemaphoreType.REGULAR((2,)),
        ],
        name="prefill",
        compiler_params=pltpu.CompilerParams(
            collective_id=0, has_side_effects=True, vmem_limit_bytes=24 * 1024 * 1024
        ),
    )(*(
        pltpu.with_memory_space_constraint(argument, pltpu.HBM)
        for argument in (
            tokens.reshape(256, 2048),
            key_weight,
            value_weight,
            queries,
            head_offset.reshape(1, 16),
            jnp.transpose(key_bias, (0, 2, 1)),
        )
    ))
    cache = jax.ShapeDtypeStruct((2, 2, 4, 128, 128), jnp.bfloat16)
    keys, values, bias, reading = pl.pallas_call(
        finish,
        out_shape=(
            cache,
            cache,
            jax.ShapeDtypeStruct((2, 2, 1024), jnp.bfloat16),
            jax.ShapeDtypeStruct((2, 128), jnp.float32),
        ),
        in_specs=[vmem] * 3,
        out_specs=(any_space,) * 4,
        scratch_shapes=[dma((4,))],
        name="finish",
        compiler_params=pltpu.CompilerParams(vmem_limit_bytes=1024 * 1024),
    )(*(pltpu.with_memory_space_constraint(part, pltpu.VMEM) for part in (held, bias, reading)))
    return (
        keys.reshape(2, 1024, 128),
        values.reshape(2, 1024, 128),
        jnp.transpose(bias, (0, 2, 1)),
        reading,
    )


def solution(mesh):
    placed = (
        P("gr", ("sp", "tp"), None),
        P("sp", None),
        P("sp", None),
        P("gr", None),
        P(),
        P("gr", ("sp", "tp"), None),
    )
    return jax.shard_map(
        per_device,
        mesh=mesh,
        in_specs=placed,
        out_specs=(P("gr", "sp", "tp"), P("gr", "sp", "tp"), P("gr", "sp", "tp"), P("gr", "tp")),
        check_vma=False,
    )
```

```python
import functools

import jax
import jax.numpy as jnp
from jax import lax
from jax.experimental import pallas as pl
from jax.experimental.pallas import tpu as pltpu
from jax.sharding import PartitionSpec as P

MESH = pl.DeviceIdType.MESH
CHUNKS = 8
EARLY = 4


def strictly_later(size):
    row = lax.broadcasted_iota(jnp.int32, (size, size), 0)
    col = lax.broadcasted_iota(jnp.int32, (size, size), 1)
    return jnp.where(row > col, 1.0, 0.0).astype(jnp.float32)


def kernel(
    tok_ref, kw_ref, vw_ref, q_hbm, off_hbm, bias_ref,
    cache_out, bias_out, read_out,
    tbuf, wa, wb, kv, bb, bsel, part, r1, mid, r2, q_ref, off_ref,
    load_sem, send, t_recv, s_recv, ay_recv, z_recv, all_recv, hello,
):
    gr, sp, tp = lax.axis_index("gr"), lax.axis_index("sp"), lax.axis_index("tp")
    zl, y = sp // 4, sp % 4
    z = gr * 8 + zl
    x, c = tp // 2, tp % 2
    px, ox = x + 1 - 2 * (x % 2), 3 - x
    half = x // 2
    ptp, otp, stp = px * 2 + c, ox * 2 + c, x * 2 + 1 - c
    dm = (x % 2) * 2 + c
    ds = (x % 2) * 2 + 1 - c
    dp = (1 - x % 2) * 2 + c
    dq = (1 - x % 2) * 2 + 1 - c

    def at_tp(t):
        return (gr, sp, t)

    def at_y(k):
        return (gr, zl * 4 + (y + k) % 4, tp)

    def at_z(k):
        there = (z + k + 16) % 16
        return (there // 8, (there % 8) * 4 + y, tp)

    def remote(src, dst, send, recv, device):
        return pltpu.make_async_remote_copy(
            src_ref=src, dst_ref=dst, send_sem=send, recv_sem=recv,
            device_id=device, device_id_type=MESH,
        )

    to_pair, along_z, along_y, to_other, of_bias, of_read1, of_read2 = range(7)

    def push(src, dst, kind, recv, device):
        remote(src, dst, send.at[kind], recv, device).start()

    tok_load = pltpu.make_async_copy(tok_ref, tbuf.at[dm], load_sem.at[0])
    tok_load.start()
    own_rows = pl.ds(pl.multiple_of(sp * 64, 64), 64)
    for n, (w_ref, lane) in enumerate(((kw_ref, 0), (vw_ref, 128))):
        for m, (buf, t) in enumerate(((wa, tp), (wb, otp))):
            cols = pl.ds(pl.multiple_of(t * 128, 128), 128)
            load = pltpu.make_async_copy(
                w_ref.at[:, cols], buf.at[own_rows, pl.ds(lane, 128)],
                load_sem.at[1],
            )
            load.start()
    bias_load = pltpu.make_async_copy(bias_ref, bb.at[tp], load_sem.at[2])
    bias_load.start()
    q_load = pltpu.make_async_copy(q_hbm, q_ref, load_sem.at[3])
    q_load.start()
    off_load = pltpu.make_async_copy(off_hbm, off_ref, load_sem.at[4])
    off_load.start()

    barrier = pltpu.get_barrier_semaphore()
    lowest, highest = z == 0, z == 15

    def greet(device):
        pl.semaphore_signal(barrier, inc=1, device_id=device, device_id_type=MESH)

    for k in (2, 1, 3):
        greet(at_y(k))
    for k in range(1, 8):
        greet(at_tp((tp + k) % 8))

    @pl.when(jnp.logical_not(highest))
    def _():
        greet(at_z(1))

    @pl.when(jnp.logical_not(lowest))
    def _():
        greet(at_z(-1))
        pl.semaphore_wait(barrier, 12)

    @pl.when(lowest)
    def _():
        pl.semaphore_wait(barrier, 11)
        greet(at_z(-1))

    @pl.when(highest)
    def _():
        greet(at_z(1))

    rows_of = 256 // CHUNKS

    def t_copy(k):
        piece = (dm, pl.ds(k * rows_of, rows_of))
        return remote(tbuf.at[piece], tbuf.at[piece], send.at[to_pair], t_recv.at[k], at_tp(ptp))

    def t_arrival(k):
        piece = (dp, pl.ds(k * rows_of, rows_of))
        return remote(tbuf.at[piece], tbuf.at[piece], send.at[to_pair], t_recv.at[k], at_tp(ptp))

    def s_sem(k):
        return s_recv.at[0 if k < EARLY else 1]

    def t_forward(k):
        piece = (dp, pl.ds(k * rows_of, rows_of))
        return remote(tbuf.at[piece], tbuf.at[piece], send.at[to_pair], s_sem(k), at_tp(stp))

    def forward_step(k):
        t_arrival(k).wait_recv()
        t_forward(k).start()

    bias_load.wait()
    for k in range(1, 8):
        push(bb.at[tp], bb.at[tp], of_bias, all_recv.at[0], at_tp((tp + k) % 8))
    tok_load.wait()
    for k in range(CHUNKS):
        t_copy(k).start()
    push(tbuf.at[dm], tbuf.at[dm], to_pair, s_recv.at[2], at_tp(stp))

    shifts = (0, 0, 1, 3, 2)

    def rows_at(offset, shift, start=0, size=64):
        block = (zl + offset + 8) % 8
        return pl.ds(pl.multiple_of(block * 256 + ((y - shift + 4) % 4) * 64 + start, 32), size)

    def z_piece(p, offset, start=0, size=64):
        return (wb if p == 0 else wa).at[rows_at(offset, shifts[p], start, size)]

    def z_push(side, p, j):
        sign = 1 if side == 0 else -1
        if j < 4:
            piece = z_piece(p, -sign * (j - 1))
        else:
            piece = z_piece(p, -sign * 3, 32 * side, 32)
        n = (side * 5 + p) * 4 + j - 1
        push(piece, piece, along_z, z_recv.at[n], at_z(sign))

    def z_wait(side, p, j):
        sign = 1 if side == 0 else -1
        piece = z_piece(p, -sign * j) if j < 4 else z_piece(p, 4, 32 * side, 32)
        n = (side * 5 + p) * 4 + j - 1
        remote(piece, piece, send.at[along_z], z_recv.at[n], at_z(sign)).wait_recv()

    def b_spread(offset):
        piece = wb.at[rows_at(offset, 0)]
        for k in (2, 1, 3):
            push(piece, piece, along_y, all_recv.at[1], at_y(k))

    pltpu.make_async_copy(kw_ref.at[:, 0:512], kw_ref.at[:, 0:512], load_sem.at[1]).wait()
    for k in (2, 1, 3):
        piece = wa.at[own_rows]
        push(piece, piece, along_y, ay_recv.at[k - 1], at_y(k))
    b_spread(0)

    @pl.when(lowest)
    def _():
        pl.semaphore_wait(barrier, 1)

    z_push(0, 0, 1)
    z_push(0, 1, 1)

    z_push(1, 0, 1)
    z_push(1, 1, 1)

    def z_step(p, j):
        for side in (0, 1):
            z_wait(side, p, j)
            if j < 4:
                z_push(side, p, j + 1)
                if p == 0:
                    b_spread(-j if side == 0 else j)
        if j == 4 and p == 0:
            b_spread(4)

    z_step(0, 1)
    for p in (2, 3, 4):
        piece = wa.at[rows_at(0, shifts[p])]
        k = shifts[p]
        remote(piece, piece, send.at[along_y], ay_recv.at[k - 1], at_y(k)).wait_recv()
        z_push(0, p, 1)
        z_push(1, p, 1)
        if p == 2:
            z_step(1, 1)
    for p in (2, 3, 4):
        z_step(p, 1)
    forward_step(0)
    for j in range(2, 5):
        for p in range(5):
            z_step(p, j)
        forward_step(j - 1)
    piece = wb.at[pl.ds(0, 24 * 64)]
    remote(piece, piece, send.at[along_y], all_recv.at[1], at_y(1)).wait_recv()

    pl.semaphore_signal(hello.at[0], inc=1, device_id=at_tp(otp), device_id_type=MESH)

    @pl.when((zl >= 2) & (zl <= 4))
    def _():
        pl.semaphore_signal(hello.at[1], inc=1, device_id=at_z(3), device_id_type=MESH)

    @pl.when((zl >= 3) & (zl <= 5))
    def _():
        pl.semaphore_signal(hello.at[1], inc=1, device_id=at_z(-3), device_id_type=MESH)

    def project(tokens, s, d, first, count):
        for g, w in enumerate((wa, wb)):
            out = jnp.dot(tokens, w[...], preferred_element_type=jnp.float32).astype(jnp.bfloat16)
            for n in range(len(d)):
                for v in (0, 1):
                    block = out[n * count : (n + 1) * count, v * 128 : (v + 1) * 128]
                    if g == 0:
                        cache_out[v, s, half, d[n], pl.ds(first, count), :] = block
                    else:
                        kv[v, s, d[n], pl.ds(first, count), :] = block

    def send_out(s, d):
        for v in (0, 1):
            push(kv.at[v, s, d], cache_out.at[v, s, half, d], to_other, all_recv.at[2], at_tp(otp))

    remote(tbuf.at[ds], tbuf.at[ds], send.at[to_pair], s_recv.at[2], at_tp(stp)).wait_recv()

    for k in range(EARLY, CHUNKS - 1):
        forward_step(k)

    def early(n, carry):
        s, which = n % 2, n // 2
        d = jnp.where(which == 0, dm, ds)
        project(tbuf[d, pl.ds(pl.multiple_of(s * 128, 128), 128), :], s, (d,), 0, 128)
        send_out(s, d)
        return carry

    lax.fori_loop(0, 4, early, 0)
    piece = (dq, pl.ds(0, EARLY * rows_of))
    remote(tbuf.at[piece], tbuf.at[piece], send.at[to_pair], s_sem(0), at_tp(stp)).wait_recv()

    def early_partner(n, carry):
        d = jnp.where(n == 0, dp, dq)
        project(tbuf[d, pl.ds(0, 128), :], 0, (d,), 0, 128)
        return carry

    lax.fori_loop(0, 2, early_partner, 0)
    forward_step(CHUNKS - 1)

    q_load.wait()
    off_load.wait()
    piece = bb.at[pl.ds(0, 7)]
    remote(piece, piece, send.at[of_bias], all_recv.at[0], at_tp(otp)).wait_recv()
    row = lax.broadcasted_iota(jnp.int32, (8, 16), 0)
    col = lax.broadcasted_iota(jnp.int32, (8, 16), 1)
    head = jnp.where(row < 2, tp, otp) * 2 + row % 2
    chosen = (col == head) & (row < 4)
    select = jnp.where(chosen, 1.0, 0.0).astype(jnp.bfloat16)
    offset = jnp.sum(
        jnp.where(chosen, jnp.broadcast_to(off_ref[...], (8, 16)), 0.0), axis=1, keepdims=True
    )
    for d in range(8):
        for s in (0, 1):
            picked = jnp.dot(select, bb[d, s], preferred_element_type=jnp.float32)
            bsel[d, s] = picked
            bias_out[s, :, d * 128 : (d + 1) * 128] = picked[0:2].astype(jnp.bfloat16)
    lane = lax.broadcasted_iota(jnp.int32, (8, 128), 1)
    row8 = lax.broadcasted_iota(jnp.int32, (8, 128), 0)
    own_lane = (lane // 64) == (row8 % 2)

    def attend(s):
        score = jnp.zeros((8, 512), jnp.float32)
        for g, t in enumerate((tp, otp)):
            cols = q_ref[:, pl.ds(pl.multiple_of(t * 128, 128), 128)].astype(jnp.float32)
            spread = jnp.broadcast_to(cols[s : s + 1], (8, 128))
            query = jnp.where(own_lane & (row8 // 2 == g), spread, 0.0).astype(jnp.bfloat16)
            keys = cache_out[0, s, half] if g == 0 else kv[0, s]
            score += lax.dot_general(
                query, keys.reshape(512, 128), (((1,), (1,)), ((), ())),
                preferred_element_type=jnp.float32,
            )
        bias = jnp.concatenate([bsel[half * 4 + d, s] for d in range(4)], axis=1)
        logit = score * 0.125 + offset + bias
        tail = jnp.log1p(jnp.exp(-jnp.abs(logit)))
        fading = -(jnp.maximum(logit, 0.0) + tail)
        ls = jnp.minimum(logit, 0.0) - tail
        blocks = [fading[:, d * 128 : (d + 1) * 128] for d in range(4)]
        within = jnp.dot(
            jnp.concatenate(blocks, axis=0), strictly_later(128),
            precision=lax.Precision.HIGHEST, preferred_element_type=jnp.float32,
        )
        carried = jnp.zeros((8, 1), jnp.float32)
        beyond = [None] * 4
        for d in (3, 2, 1, 0):
            beyond[d] = within[d * 8 : d * 8 + 8] + carried
            carried = carried + jnp.sum(blocks[d], axis=1, keepdims=True)
        weight = jnp.exp(ls + jnp.concatenate(beyond, axis=1))
        high = weight.astype(jnp.bfloat16)
        low = (weight - high.astype(jnp.float32)).astype(jnp.bfloat16)
        both = jnp.concatenate([high, low], axis=0)
        sums = jnp.where(own_lane, jnp.broadcast_to(carried, (8, 128)), 0.0)
        for g in (0, 1):
            values = cache_out[1, s, half] if g == 0 else kv[1, s]
            product = jnp.dot(both, values.reshape(512, 128), preferred_element_type=jnp.float32)
            mixture = jnp.where(own_lane, product[0:8] + product[8:16], 0.0)
            r = 2 * g
            part[g, s : s + 1, :] = mixture[r : r + 1] + mixture[r + 1 : r + 2]
            part[g, 2 + s : 3 + s, :] = sums[r : r + 1] + sums[r + 1 : r + 2]

    attend(0)

    piece = (dq, pl.ds(EARLY * rows_of, 128))
    remote(tbuf.at[piece], tbuf.at[piece], send.at[to_pair], s_recv.at[1], at_tp(stp)).wait_recv()

    def late(n, carry):
        d = jnp.where(n == 0, dp, dq)
        project(tbuf[d, pl.ds(128, 128), :], 1, (d,), 0, 128)
        return carry

    lax.fori_loop(0, 2, late, 0)
    attend(1)
    pl.semaphore_wait(hello.at[0], 1)

    @pl.when((zl <= 2) | (zl >= 5))
    def _():
        pl.semaphore_wait(hello.at[1], 1)

    mine = y * 2 + half
    for k in (2, 1, 3):
        push(part.at[1], r1.at[mine], of_read1, all_recv.at[3], (gr, zl * 4 + (y + k) % 4, otp))
        push(part.at[0], r1.at[mine], of_read1, all_recv.at[3], at_y(k))
    push(part.at[1], r1.at[mine], of_read1, all_recv.at[3], at_tp(otp))
    r1[mine] = part[0]
    for s in (0, 1):
        send_out(s, dp)
        send_out(s, dq)
    piece = r1.at[pl.ds(0, 7)]
    remote(piece, piece, send.at[of_read1], all_recv.at[3], at_tp(otp)).wait_recv()

    def combine(buf):
        total = buf[7][2:4]
        mixed = buf[7][0:2]
        for n in range(6, -1, -1):
            block = buf[n]
            mixed = mixed + block[0:2] * jnp.exp(total)
            total = total + block[2:4]
        return mixed, total

    mixed, total = combine(r1)
    mid[...] = jnp.concatenate([mixed, total], axis=0)
    r2[zl] = jnp.concatenate([mixed, total], axis=0)
    for k in range(7, 0, -1):
        push(mid, r2.at[zl], of_read2, all_recv.at[4], (gr, ((zl + k) % 8) * 4 + y, tp))
    piece = r2.at[pl.ds(0, 7)]
    remote(piece, piece, send.at[of_read2], all_recv.at[4], at_z(1)).wait_recv()
    mixed, total = combine(r2)
    square = mixed * mixed
    first_head = lax.broadcasted_iota(jnp.int32, (2, 128), 1) < 64
    mean_a = jnp.sum(jnp.where(first_head, square, 0.0), axis=1, keepdims=True) * (1.0 / 64)
    mean_b = jnp.sum(jnp.where(first_head, 0.0, square), axis=1, keepdims=True) * (1.0 / 64)
    read_out[...] = mixed * lax.rsqrt(jnp.where(first_head, mean_a, mean_b) + 1e-06)

    remote(kv, kv, send.at[to_other], all_recv.at[2], at_tp(otp)).wait_recv()
    for kind, whole in (
        (to_pair, tbuf.at[pl.ds(0, 3)]),
        (along_z, tbuf.at[:, pl.ds(0, 224), pl.ds(0, 640)]),
        (along_y, tbuf.at[:, pl.ds(0, 144), pl.ds(0, 768)]),
        (to_other, kv),
        (of_bias, bb.at[pl.ds(0, 7)]),
        (of_read1, r1.at[pl.ds(0, 7)]),
        (of_read2, r2.at[pl.ds(0, 7)]),
    ):
        remote(whole, whole, send.at[kind], all_recv.at[0], at_tp(otp)).wait_send()


def finish(cache_ref, bias_ref, read_ref, key_out, value_out, bias_out, read_out, sem):
    pairs = (
        (cache_ref.at[0], key_out), (cache_ref.at[1], value_out),
        (bias_ref, bias_out), (read_ref, read_out),
    )
    copies = [pltpu.make_async_copy(src, dst, sem.at[n]) for n, (src, dst) in enumerate(pairs)]
    for copy in copies:
        copy.start()
    for copy in copies:
        copy.wait()


def per_device(tokens, key_weight, value_weight, queries, head_offset, key_bias):
    any_space = pl.BlockSpec(memory_space=pl.ANY)
    vmem = pl.BlockSpec(memory_space=pltpu.VMEM)
    dma = pltpu.SemaphoreType.DMA
    held, bias, reading = pl.pallas_call(
        kernel,
        out_shape=(
            pltpu.VMEM((2, 2, 2, 4, 128, 128), jnp.bfloat16),
            pltpu.VMEM((2, 2, 1024), jnp.bfloat16),
            pltpu.VMEM((2, 128), jnp.float32),
        ),
        in_specs=[any_space] * 6,
        out_specs=(vmem, vmem, vmem),
        scratch_shapes=[
            pltpu.VMEM((4, 256, 2048), jnp.bfloat16),
            pltpu.VMEM((2048, 256), jnp.bfloat16),
            pltpu.VMEM((2048, 256), jnp.bfloat16),
            pltpu.VMEM((2, 2, 4, 128, 128), jnp.bfloat16),
            pltpu.VMEM((8, 2, 16, 128), jnp.bfloat16),
            pltpu.VMEM((8, 2, 8, 128), jnp.float32),
            pltpu.VMEM((2, 4, 128), jnp.float32),
            pltpu.VMEM((8, 4, 128), jnp.float32),
            pltpu.VMEM((4, 128), jnp.float32),
            pltpu.VMEM((8, 4, 128), jnp.float32),
            pltpu.VMEM((2, 1024), jnp.bfloat16),
            pltpu.VMEM((1, 16), jnp.float32),
            dma((5,)), dma((7,)),
            dma((CHUNKS,)), dma((3,)), dma((3,)), dma((40,)), dma((5,)),
            pltpu.SemaphoreType.REGULAR((2,)),
        ],
        name="prefill",
        compiler_params=pltpu.CompilerParams(
            collective_id=0, has_side_effects=True, vmem_limit_bytes=24 * 1024 * 1024
        ),
    )(*(
        pltpu.with_memory_space_constraint(argument, pltpu.HBM)
        for argument in (
            tokens.reshape(256, 2048),
            key_weight,
            value_weight,
            queries,
            head_offset.reshape(1, 16),
            jnp.transpose(key_bias, (0, 2, 1)),
        )
    ))
    cache = jax.ShapeDtypeStruct((2, 2, 4, 128, 128), jnp.bfloat16)
    keys, values, bias, reading = pl.pallas_call(
        finish,
        out_shape=(
            cache,
            cache,
            jax.ShapeDtypeStruct((2, 2, 1024), jnp.bfloat16),
            jax.ShapeDtypeStruct((2, 128), jnp.float32),
        ),
        in_specs=[vmem] * 3,
        out_specs=(any_space,) * 4,
        scratch_shapes=[dma((4,))],
        name="finish",
        compiler_params=pltpu.CompilerParams(vmem_limit_bytes=1024 * 1024),
    )(*(pltpu.with_memory_space_constraint(part, pltpu.VMEM) for part in (held, bias, reading)))
    return (
        keys.reshape(2, 1024, 128),
        values.reshape(2, 1024, 128),
        jnp.transpose(bias, (0, 2, 1)),
        reading,
    )


def solution(mesh):
    placed = (
        P("gr", ("sp", "tp"), None),
        P("sp", None),
        P("sp", None),
        P("gr", None),
        P(),
        P("gr", ("sp", "tp"), None),
    )
    return jax.shard_map(
        per_device,
        mesh=mesh,
        in_specs=placed,
        out_specs=(P("gr", "sp", "tp"), P("gr", "sp", "tp"), P("gr", "sp", "tp"), P("gr", "tp")),
        check_vma=False,
    )
```
